32 devices in a mesh: ep: 8 (over z, y), tp: 4 (over x, core).
Axes of the slice: x: 2, y: 2, z: 4, core: 2. Of those that a mesh axis runs over, the one named last changes fastest.
Arguments:
- queries: bfloat16 [4096, 1024], P('ep', 'tp'), may hold values from -6 to 6
- key_rows: bfloat16 [4096, 512], P('ep', 'tp'), may hold values from -6 to 6
- value_rows: bfloat16 [4096, 512], P('ep', 'tp'), may hold values from -6 to 6
- forget_logit: float32 [8, 4096], P('tp', 'ep'), may hold values from -1 to 17
- out_weight: bfloat16 [1024, 2048], P('tp'), may hold values from -0.1875 to 0.1875
- out_gain: float32 [2048], replicated, may hold values from 0.1 to 1.9
- moe_input: bfloat16 [4096, 2048], P('ep'), may hold values from -6 to 6
- moe_gain: float32 [2048], replicated, may hold values from 0.1 to 1.9
- router_group: bfloat16 [2048, 4], replicated, may hold values from -2 to 2
- router_expert: bfloat16 [2048, 8], replicated, may hold values from -0.125 to 0.125
- route_group: int32 [4096], P('ep'), may hold values from 0 to 3
- route_pick: int32 [4096, 2], P('ep'), may hold values from 0 to 1, as said below
- expert_gate: bfloat16 [8, 2048, 1024], P('ep', None, 'tp'), may hold values from -0.125 to 0.125
- expert_up: bfloat16 [8, 2048, 1024], P('ep', None, 'tp'), may hold values from -0.125 to 0.125
- expert_down: bfloat16 [8, 1024, 2048], P('ep', 'tp'), may hold values from -42 to 42
Outputs:
- mixer_out: bfloat16 [4096, 2048], P(('ep', 'tp'))
- moe_out: bfloat16 [4096, 2048], P(('ep', 'tp'))
The draws below stay inside these ranges and needn't reach their ends.
Inputs may be any that keep to these rules, and one draw needn't show every extreme that they name: `route_pick`: the two entries of a row differ.
All inputs are finite; a program needn't handle non-finite values.
Results may differ from the reference program's by a relative error of at most 0.013.
Values may be sent and summed in bfloat16 or wider, within the bound.
A program may use at most 128 MiB of HBM per device.

```python
import math
import jax
import jax.numpy as jnp
from jax import lax

D = 2048
H = 8
KVH = 4
DH = 128
FF = 1024
GROUPS = 4
TOK_DEV = 128
EXPERTS = 8
CAPD = 64
TOKENS_A = 4096
TOKENS_B = 4096
N_TP = 4


def draw_queries(key, part):
    own_key = jax.random.fold_in(key, 21)
    values = jnp.clip(jax.random.normal(own_key, (TOKENS_A, H * DH), jnp.float32), -6.0, 6.0)
    return values.astype(jnp.bfloat16)


def draw_key_rows(key, part):
    own_key = jax.random.fold_in(key, 22)
    values = jnp.clip(jax.random.normal(own_key, (TOKENS_A, KVH * DH), jnp.float32), -6.0, 6.0)
    return values.astype(jnp.bfloat16)


def draw_forget_logit(key, part):
    order_key, block_key, noise_key = jax.random.split(jax.random.fold_in(key, 31), 3)
    ranking = jax.random.permutation(order_key, H)
    slow = ranking >= H // 2
    base = jnp.where(slow, jnp.log(1.0 * TOKENS_A), jnp.log(50.0))
    shift = jax.random.uniform(block_key, (H, EXPERTS), jnp.float32, -0.8, 0.8)
    shift = jnp.repeat(shift, TOKENS_A // EXPERTS, axis=1)
    noise = 0.7 * jnp.clip(jax.random.normal(noise_key, (H, TOKENS_A), jnp.float32), -4.0, 4.0)
    return (base[:, None] + shift + noise).astype(jnp.float32)


def group_directions(key):
    sign_key, common_key = jax.random.split(jax.random.fold_in(key, 43))
    directions = jnp.where(jax.random.randint(sign_key, (GROUPS, D), 0, 2) == 0, -1.0, 1.0)
    common = jnp.where(jax.random.randint(common_key, (D,), 0, 2) == 0, -1.0, 1.0)
    return (directions.astype(jnp.float32), common.astype(jnp.float32))


def routing(key):
    base = jax.random.fold_in(key, 61)
    group_key, first_key, second_key, hot_key, pick_key, order_key = jax.random.split(base, 6)
    per_group = EXPERTS // GROUPS
    groups = jax.random.randint(group_key, (TOKENS_B,), 0, GROUPS)
    first = jax.random.randint(first_key, (TOKENS_B,), 0, per_group)
    offset = jax.random.randint(second_key, (TOKENS_B,), 0, per_group - 1)
    hot_group = jax.random.randint(hot_key, (), 0, GROUPS)
    hot_pick = jax.random.randint(pick_key, (), 0, per_group)
    blocks = TOKENS_B // TOK_DEV
    scores = jax.random.randint(order_key, (blocks, TOK_DEV), 0, 1 << 20) * TOK_DEV
    scores = scores + jnp.arange(TOK_DEV, dtype=jnp.int32)[None, :]
    ranking = jnp.argsort(jnp.argsort(scores, axis=1), axis=1).reshape(-1)
    forced = ranking < CAPD
    groups = jnp.where(forced, hot_group, groups)
    first = jnp.where(forced, hot_pick, first)
    second = (first + 1 + offset) % per_group
    return (groups.astype(jnp.int32), jnp.stack([first, second], axis=1).astype(jnp.int32))


def draw_moe_input(key, part):
    groups = routing(key)[0]
    directions, common = group_directions(key)
    noise_key = jax.random.fold_in(key, 41)
    level_key, jitter_key, mark_key, sign_key = jax.random.split(jax.random.fold_in(key, 44), 4)
    noise = jnp.clip(jax.random.normal(noise_key, (TOKENS_B, D), jnp.float32), -4.0, 4.0)
    level = jax.random.uniform(level_key, (TOKENS_B, 1), jnp.float32, 0.35, 0.7)
    jitter = jax.random.uniform(jitter_key, (TOKENS_B, GROUPS), jnp.float32, 0.8, 1.2)
    routed = jnp.arange(GROUPS, dtype=jnp.int32)[None, :] == groups[:, None]
    amounts = level * jnp.where(routed, -1.0, jitter)
    values = noise + jnp.dot(amounts, directions, precision=lax.Precision.HIGHEST)
    return jnp.clip(values, -6.0, 6.0).astype(jnp.bfloat16)


def draw_router_group(key, part):
    directions, common = group_directions(key)
    own_key = jax.random.fold_in(key, 51)
    noise = 0.2 * jnp.clip(jax.random.normal(own_key, (D, GROUPS), jnp.float32), -6.0, 6.0) / jnp.sqrt(1.0 * D)
    values = noise + 5.0 * directions.T / D
    return values.astype(jnp.bfloat16)


def draw_route_group(key, part):
    return routing(key)[0]


def draw_route_pick(key, part):
    return routing(key)[1]


def block_scale(key, shape, shards, smallest, largest):
    loudness, own = 1.0, jax.random.fold_in(key, 6)
    for dim, blocks in shards:
        heights = jnp.exp(jax.random.uniform(jax.random.fold_in(own, dim), (blocks,), jnp.float32, smallest / len(shards), largest / len(shards)))
        loudness = loudness * jnp.repeat(heights, shape[dim] // blocks).reshape([-1 if axis == dim else 1 for axis in range(len(shape))])
    return loudness


def normal_values(key, dims, deviation, bound, pieces=(), kind=jnp.bfloat16):
    factor_of = block_scale(key, dims, pieces, -0.22, 0.18) if pieces else 1.0
    values = jax.random.normal(key, dims, jnp.float32) * deviation * factor_of
    return jnp.minimum(jnp.maximum(values, -bound), bound).astype(kind)


def setup_inputs(seed: int = 0) -> dict:
    seeds = jax.random.split(jax.random.key(seed), 16)
    queries = draw_queries(jax.random.fold_in(seeds[15], 71), 0)
    key_rows = draw_key_rows(jax.random.fold_in(seeds[15], 71), 0)
    value_rows = normal_values(seeds[2], (TOKENS_A, KVH * DH), 1.0, 6.0, ((0, 8), (1, 4)))
    forget_logit = draw_forget_logit(jax.random.fold_in(seeds[15], 71), 0)
    out_weight = normal_values(seeds[4], (H * DH, D), (H * DH) ** -0.5, 0.1875, ((0, 4),))
    out_gain = jnp.clip(1.0 + 0.18 * jax.random.normal(seeds[5], (D,), jnp.float32), 0.1, 1.9)
    moe_input = draw_moe_input(jax.random.fold_in(seeds[15], 71), 0)
    moe_gain = jnp.clip(1.0 + 0.18 * jax.random.normal(seeds[7], (D,), jnp.float32), 0.1, 1.9)
    router_group = draw_router_group(jax.random.fold_in(seeds[15], 71), 0)
    router_expert = normal_values(seeds[9], (D, EXPERTS), D ** -0.5, 0.125)
    route_group = draw_route_group(jax.random.fold_in(seeds[15], 71), 0)
    route_pick = draw_route_pick(jax.random.fold_in(seeds[15], 71), 0)
    expert_gate = normal_values(seeds[12], (EXPERTS, D, FF), D ** -0.5, 0.125, ((0, 8), (2, 4)))
    expert_up = normal_values(seeds[13], (EXPERTS, D, FF), D ** -0.5, 0.125, ((0, 8), (2, 4)))
    expert_down = normal_values(seeds[14], (EXPERTS, FF, D), 7.0, 42.0, ((0, 8), (1, 4)))
    return {"queries": queries, "key_rows": key_rows, "value_rows": value_rows, "forget_logit": forget_logit, "out_weight": out_weight, "out_gain": out_gain, "moe_input": moe_input, "moe_gain": moe_gain, "router_group": router_group, "router_expert": router_expert, "route_group": route_group, "route_pick": route_pick, "expert_gate": expert_gate, "expert_up": expert_up, "expert_down": expert_down}


def rms_scale(row_block, scale_gain):
    values = row_block.astype(jnp.float32)
    return values * lax.rsqrt(lax.optimization_barrier(jnp.mean(values * values, axis=-1, keepdims=True)) + 1e-06) * scale_gain

def slot_ranks(chosen, block_rows, experts):
    expert_ids = jnp.arange(experts, dtype=jnp.int32)
    matches = chosen[:, :, None] == expert_ids
    usage = jnp.any(matches, axis=1).astype(jnp.int32)
    grouped = usage.reshape(-1, block_rows, experts)
    before = (jnp.cumsum(grouped, axis=1) - grouped).reshape(-1, experts)
    return lax.optimization_barrier(jnp.sum(jnp.where(matches, before[:, None, :], 0), axis=2)).astype(jnp.int32)

def reference(queries, key_rows, value_rows, forget_logit, out_weight, out_gain, moe_input, moe_gain, router_group, router_expert, route_group, route_pick, expert_gate, expert_up, expert_down):
    length = TOKENS_A
    ratio = H // KVH
    cum_gate = jnp.cumsum(jax.nn.log_sigmoid(forget_logit), axis=1)
    query_heads = queries.reshape(length, H, DH)
    key_heads = key_rows.reshape(length, KVH, DH)
    value_heads = value_rows.reshape(length, KVH, DH)
    block_len = math.gcd(512, length)
    positions = jnp.arange(length, dtype=jnp.int32)

    def one_block(block_index):
        start = (block_index * block_len).astype(jnp.int32)
        query_block = lax.dynamic_slice_in_dim(query_heads, start, block_len, 0)
        cum_block = lax.dynamic_slice_in_dim(cum_gate, start, block_len, 1)
        query_pos = start + jnp.arange(block_len, dtype=jnp.int32)
        visible = positions[None, :] <= query_pos[:, None]
        results = []
        for head_index in range(H):
            shared = head_index // ratio
            scores = jnp.dot(query_block[:, head_index], key_heads[:, shared].T, preferred_element_type=jnp.float32) / math.sqrt(DH)
            scores = scores + cum_block[head_index][:, None] - cum_gate[head_index][None, :]
            scores = jnp.where(visible, scores, -jnp.inf)
            row_top = lax.optimization_barrier(jnp.max(scores, axis=1, keepdims=True))
            expo = jnp.exp(scores - row_top)
            row_total = lax.optimization_barrier(jnp.sum(expo, axis=1, keepdims=True))
            weighted = jnp.dot(expo.astype(jnp.bfloat16), value_heads[:, shared], preferred_element_type=jnp.float32)
            results.append((weighted / row_total).astype(jnp.bfloat16))
        return jnp.concatenate(results, axis=1)
    attended = lax.map(one_block, jnp.arange(length // block_len, dtype=jnp.int32)).reshape(length, H * DH)
    block_width = H * DH // N_TP
    projected = jnp.zeros((length, D), jnp.float32)
    for portion in range(N_TP):
        piece = jnp.dot(attended[:, portion * block_width:(portion + 1) * block_width], out_weight[portion * block_width:(portion + 1) * block_width], preferred_element_type=jnp.float32).astype(jnp.bfloat16)
        projected = projected + lax.optimization_barrier(piece).astype(jnp.float32)
    mixer_out = rms_scale(projected, out_gain).astype(jnp.bfloat16)
    tokens = TOKENS_B
    experts = EXPERTS
    per_group = experts // GROUPS
    normed = rms_scale(moe_input, moe_gain).astype(jnp.bfloat16)
    group_logits = jnp.dot(normed, router_group, preferred_element_type=jnp.float32)
    expert_logits = jnp.dot(normed, router_expert, preferred_element_type=jnp.float32)
    group_top = lax.optimization_barrier(jnp.max(group_logits, axis=1, keepdims=True))
    group_exp = jnp.exp(group_logits - group_top)
    group_hit = jnp.arange(GROUPS, dtype=jnp.int32)[None, :] == route_group[:, None]
    group_share = lax.optimization_barrier(jnp.sum(jnp.where(group_hit, group_exp, 0.0), axis=1)) / lax.optimization_barrier(jnp.sum(group_exp, axis=1))
    chosen = (route_group[:, None] * per_group + route_pick).astype(jnp.int32)
    expert_hit = jnp.arange(experts, dtype=jnp.int32)[None, None, :] == chosen[:, :, None]
    picked_logits = lax.optimization_barrier(jnp.sum(jnp.where(expert_hit, expert_logits[:, None, :], 0.0), axis=2))
    shares = group_share[:, None] * jax.nn.sigmoid(picked_logits - picked_logits[:, ::-1])
    slot_rank = slot_ranks(chosen, TOK_DEV, experts)
    is_kept = slot_rank < CAPD
    slots = tokens // TOK_DEV * CAPD
    block_of = (jnp.arange(tokens, dtype=jnp.int32) // TOK_DEV)[:, None]
    slot_pos = (block_of * CAPD + slot_rank).astype(jnp.int32)
    target = jnp.where(is_kept, chosen * slots + slot_pos, experts * slots).astype(jnp.int32)
    sources = jnp.broadcast_to(jnp.arange(tokens, dtype=jnp.int32)[:, None], target.shape)
    slot_table = jnp.full((experts * slots,), tokens, jnp.int32).at[target.reshape(-1)].set(sources.reshape(-1), mode='drop').reshape(experts, slots)
    padded = jnp.concatenate([normed, jnp.zeros((1, D), jnp.bfloat16)], axis=0)
    quarter = FF // N_TP

    def one_expert(inputs):
        table_row, gate_w, up_w, down_w = inputs
        gathered = padded[table_row]
        gated = jnp.dot(gathered, gate_w, preferred_element_type=jnp.float32)
        lifted = jnp.dot(gathered, up_w, preferred_element_type=jnp.float32)
        hidden = (jax.nn.silu(gated) * lifted).astype(jnp.bfloat16)
        summed = jnp.zeros((slots, D), jnp.float32)
        for portion in range(N_TP):
            piece = jnp.dot(hidden[:, portion * quarter:(portion + 1) * quarter], down_w[portion * quarter:(portion + 1) * quarter], preferred_element_type=jnp.float32).astype(jnp.bfloat16)
            summed = summed + lax.optimization_barrier(piece).astype(jnp.float32)
        return summed.astype(jnp.bfloat16)
    results = lax.map(one_expert, (slot_table, expert_gate, expert_up, expert_down)).reshape(experts * slots, D)
    slot_index = jnp.where(is_kept, chosen * slots + slot_pos, 0).astype(jnp.int32)
    picked = results[slot_index]
    moe_out = lax.optimization_barrier(jnp.sum(jnp.where(is_kept, shares, 0.0)[:, :, None] * picked.astype(jnp.float32), axis=1))
    return (mixer_out, moe_out.astype(jnp.bfloat16))
```

```python
import functools
import math

import jax
import jax.numpy as jnp
from jax import lax
from jax.experimental import pallas as pl
from jax.experimental.pallas import tpu as pltpu
from jax.sharding import PartitionSpec as P

DH = 128
GROUPS = 4


def rms_scale(row_block, scale_gain):
    values = row_block.astype(jnp.float32)
    return (
        values * lax.rsqrt(jnp.mean(values * values, axis=-1, keepdims=True) + 1e-06) * scale_gain
    )


def slot_ranks(chosen, block_rows, experts):
    expert_ids = jnp.arange(experts, dtype=jnp.int32)
    matches = chosen[:, :, None] == expert_ids
    usage = jnp.any(matches, axis=1).astype(jnp.int32)
    grouped = usage.reshape(-1, block_rows, experts)
    before = (jnp.cumsum(grouped, axis=1) - grouped).reshape(-1, experts)
    return jnp.sum(jnp.where(matches, before[:, None, :], 0), axis=2)


def expert_hidden(arrived, gate_part, up_part):
    flat = arrived.reshape(-1, arrived.shape[-1])
    gated = jnp.dot(flat, gate_part, preferred_element_type=jnp.float32)
    lifted = jnp.dot(flat, up_part, preferred_element_type=jnp.float32)
    hidden = (jax.nn.silu(gated) * lifted).astype(jnp.bfloat16)
    return hidden.reshape(arrived.shape[:-1] + (gate_part.shape[1],))


def general_body(
    queries,
    key_rows,
    value_rows,
    forget_logit,
    out_weight,
    out_gain,
    moe_input,
    moe_gain,
    router_group,
    router_expert,
    route_group,
    route_pick,
    expert_gate,
    expert_up,
    expert_down,
):
    tp_count = lax.axis_size("tp")
    ep_count = lax.axis_size("ep")
    tp_index = lax.axis_index("tp")
    ep_index = lax.axis_index("ep")
    rows_group = queries.shape[0]
    query_heads = forget_logit.shape[0]
    key_heads = key_rows.shape[1] // DH
    ratio = query_heads // key_heads
    own_start = ep_index * rows_group
    own_pos = own_start + jnp.arange(rows_group, dtype=jnp.int32)
    local_cum = jnp.cumsum(jax.nn.log_sigmoid(forget_logit), axis=1)
    every_cum = lax.all_gather(local_cum, "ep", axis=1, tiled=True).reshape(
        query_heads, ep_count, rows_group
    )
    shard_totals = every_cum[:, :, -1]
    offsets = jnp.cumsum(shard_totals, axis=1) - shard_totals
    cum_gate = (every_cum + offsets[:, :, None]).reshape(query_heads, ep_count * rows_group)
    own_cum = lax.dynamic_slice_in_dim(cum_gate, own_start, rows_group, 1).reshape(
        key_heads, ratio, rows_group, 1
    )
    query_stack = (
        queries.reshape(rows_group, key_heads, ratio, DH)
        .transpose(1, 2, 0, 3)
        .reshape(key_heads, ratio * rows_group, DH)
    )

    def attend_block(current, keys_block, values_block, start):
        piece_rows = keys_block.shape[0]

        def compute(state):
            row_top, row_total, weighted = state
            key_stack = keys_block.reshape(piece_rows, key_heads, DH).transpose(1, 0, 2)
            value_stack = values_block.reshape(piece_rows, key_heads, DH).transpose(1, 0, 2)
            scores = jnp.einsum(
                "gqd,gkd->gqk", query_stack, key_stack, preferred_element_type=jnp.float32
            ) / math.sqrt(DH)
            key_cum = lax.dynamic_slice_in_dim(cum_gate, start, piece_rows, 1).reshape(
                key_heads, ratio, 1, piece_rows
            )
            logits = scores.reshape(key_heads, ratio, rows_group, piece_rows) + own_cum - key_cum
            visible = (start + jnp.arange(piece_rows, dtype=jnp.int32))[None, :] <= own_pos[:, None]
            logits = jnp.where(visible, logits, -1e30)
            new_top = jnp.maximum(row_top, jnp.max(logits, axis=3))
            expo = jnp.where(visible, jnp.exp(logits - new_top[..., None]), 0.0)
            rescale = jnp.exp(row_top - new_top)
            row_total = row_total * rescale + jnp.sum(expo, axis=3)
            product = jnp.einsum(
                "gqk,gkd->gqd",
                expo.reshape(key_heads, ratio * rows_group, piece_rows).astype(jnp.bfloat16),
                value_stack,
                preferred_element_type=jnp.float32,
            )
            weighted = weighted * rescale.reshape(key_heads, ratio * rows_group, 1) + product
            return (new_top, row_total, weighted)

        return lax.cond(start < own_start + rows_group, compute, lambda state: state, current)

    initial = (
        jnp.full((key_heads, ratio, rows_group), -1e30, jnp.float32),
        jnp.zeros((key_heads, ratio, rows_group), jnp.float32),
        jnp.zeros((key_heads, ratio * rows_group, DH), jnp.float32),
    )
    current = initial
    keys_piece = lax.all_gather(key_rows, "ep", axis=0, tiled=True)
    values_piece = lax.all_gather(value_rows, "ep", axis=0, tiled=True)
    piece_rows = keys_piece.shape[0]
    blocks = piece_rows // rows_group

    def advance(state, inputs):
        keys_block, values_block, block_index = inputs
        return (attend_block(state, keys_block, values_block, block_index * rows_group), None)

    current, _ = lax.scan(
        advance,
        current,
        (
            keys_piece.reshape(blocks, rows_group, -1),
            values_piece.reshape(blocks, rows_group, -1),
            jnp.arange(blocks, dtype=jnp.int32),
        ),
    )
    row_top, row_total, weighted = current
    attended = (weighted / row_total.reshape(key_heads, ratio * rows_group, 1)).astype(jnp.bfloat16)
    attended = (
        attended.reshape(key_heads, ratio, rows_group, DH)
        .transpose(2, 0, 1, 3)
        .reshape(rows_group, query_heads * DH)
    )
    group_rows = moe_input.shape[0]
    own_rows = group_rows // tp_count
    width_model = moe_input.shape[1]
    experts = expert_gate.shape[0] * ep_count
    per_group = experts // GROUPS
    capacity = tp_count * own_rows // experts
    own_first = tp_index * own_rows
    chosen_all = route_group[:, None] * per_group + route_pick
    rank_all = slot_ranks(chosen_all, own_rows, experts)
    chosen = lax.dynamic_slice_in_dim(chosen_all, own_first, own_rows, 0)
    ranks = lax.dynamic_slice_in_dim(rank_all, own_first, own_rows, 0)
    is_kept = ranks < capacity
    own_group = lax.dynamic_slice_in_dim(route_group, own_first, own_rows, 0)
    normed = rms_scale(
        lax.dynamic_slice_in_dim(moe_input, own_first, own_rows, 0), moe_gain
    ).astype(jnp.bfloat16)
    target = jnp.where(is_kept, chosen * capacity + ranks, experts * capacity)
    sources = jnp.broadcast_to(jnp.arange(own_rows, dtype=jnp.int32)[:, None], target.shape)
    slot_table = (
        jnp.full((experts * capacity,), own_rows, jnp.int32)
        .at[target.reshape(-1)]
        .set(sources.reshape(-1), mode="drop")
    )
    padded = jnp.concatenate([normed, jnp.zeros((1, width_model), jnp.bfloat16)], axis=0)
    outgoing = padded[slot_table].reshape(experts, capacity, width_model)
    arrived = lax.all_to_all(outgoing, "ep", split_axis=0, concat_axis=0, tiled=True)
    hidden_arrived = lax.all_gather(arrived[None], "tp", axis=0, tiled=True)
    hidden = expert_hidden(hidden_arrived, expert_gate[0], expert_up[0])
    hidden_rows = hidden.reshape(-1, hidden.shape[-1])
    mixer_term = jnp.dot(attended, out_weight, preferred_element_type=jnp.float32)
    expert_term = jnp.dot(hidden_rows, expert_down[0], preferred_element_type=jnp.float32)
    mixer_summed, expert_summed = (
        lax.psum_scatter(
            mixer_term.astype(jnp.bfloat16), "tp", scatter_dimension=0, tiled=True
        ).astype(jnp.float32),
        lax.psum_scatter(
            expert_term.astype(jnp.bfloat16), "tp", scatter_dimension=0, tiled=True
        ).astype(jnp.float32),
    )
    mixer_out = rms_scale(mixer_summed, out_gain).astype(jnp.bfloat16)
    group_logits = jnp.dot(normed, router_group, preferred_element_type=jnp.float32)
    expert_logits = jnp.dot(normed, router_expert, preferred_element_type=jnp.float32)
    group_top = jnp.max(group_logits, axis=1, keepdims=True)
    group_exp = jnp.exp(group_logits - group_top)
    group_hit = jnp.arange(GROUPS, dtype=jnp.int32)[None, :] == own_group[:, None]
    group_share = jnp.sum(jnp.where(group_hit, group_exp, 0.0), axis=1) / jnp.sum(group_exp, axis=1)
    expert_hit = jnp.arange(experts, dtype=jnp.int32)[None, None, :] == chosen[:, :, None]
    picked_logits = jnp.sum(jnp.where(expert_hit, expert_logits[:, None, :], 0.0), axis=2)
    shares = group_share[:, None] * jax.nn.sigmoid(picked_logits - picked_logits[:, ::-1])
    results = expert_summed.astype(jnp.bfloat16).reshape(ep_count, capacity, width_model)
    returned = lax.all_to_all(results, "ep", split_axis=0, concat_axis=0, tiled=True).reshape(
        experts * capacity, width_model
    )
    slot_index = jnp.where(is_kept, chosen * capacity + ranks, 0)
    picked = returned[slot_index]
    moe_out = jnp.sum(
        jnp.where(is_kept, shares, 0.0)[:, :, None] * picked.astype(jnp.float32), axis=1
    )
    return (mixer_out, moe_out.astype(jnp.bfloat16))


LOG2E = math.log2(math.e)
MESH = pl.DeviceIdType.MESH
VMEM = pl.BlockSpec(memory_space=pltpu.VMEM)
ANY = pl.BlockSpec(memory_space=pl.ANY)


def places():
    ep, tp = lax.axis_index("ep"), lax.axis_index("tp")
    return ep, tp, ep // 2, ep % 2, tp // 2, tp % 2


def greet(groups):
    ep, tp, z, y, x, c = places()
    barrier = pltpu.get_barrier_semaphore()
    peers = [(z * 2 + 1 - y, tp), (ep, (1 - x) * 2 + c), (ep, x * 2 + 1 - c)]
    peers += [(lax.rem(z + d, groups) * 2 + y, tp) for d in range(1, groups)]
    for peer in peers:
        pl.semaphore_signal(barrier, inc=1, device_id=peer, device_id_type=MESH)
    pl.semaphore_wait(barrier, len(peers))


def remote(src, dst, send, recv, peer):
    return pltpu.make_async_remote_copy(
        src_ref=src, dst_ref=dst, send_sem=send, recv_sem=recv, device_id=peer, device_id_type=MESH
    )


def dispatch_kernel(
    groups, slots, keys, vals, cum, gate, up, down,
    rows, keys_all, vals_all, cum_all, gate_o, up_o, down_o,
    local_sem, kvz_s, kvz_r, kvy_s, kvy_r, w_s, w_r, z_s, z_r, y_s, y_r, x_s, x_r,
):
    ep, tp, z, y, x, c = places()
    greet(groups)
    across_y = (z * 2 + 1 - y, tp)
    across_x = (ep, (1 - x) * 2 + c)
    across_c = (ep, x * 2 + 1 - c)
    own = x * 2 + y
    beside = x * 2 + 1 - y
    stream = ((keys, keys_all), (vals, vals_all), (cum, cum_all))

    for i, (src, dst) in enumerate(stream):
        for d in range(1, groups):
            @pl.when(z + d < groups)
            def _(i=i, src=src, dst=dst, d=d):
                remote(
                    src, dst.at[ep], kvz_s.at[i, d], kvz_r.at[i, d],
                    (lax.rem(z + d, groups) * 2 + y, tp),
                ).start()

    def z_copy(d):
        to = lax.rem(z + d, groups)
        return remote(slots.at[to], rows.at[own, z], z_s.at[d], z_r.at[d], (to * 2 + y, tp))

    def chunk(q, d):
        return rows.at[q, lax.rem(z - d + groups, groups)]

    for d in range(1, groups):
        z_copy(d).start()

    def y_copy(d):
        src = slots.at[z] if d == 0 else chunk(own, d)
        return remote(src, chunk(own, d), y_s.at[d], y_r.at[d], across_y)

    def x_copy(d):
        src = slots.at[z] if d == 0 else chunk(own, d)
        return remote(src, chunk(own, d), x_s.at[0, d], x_r.at[0, d], across_x)

    def x_relay(d):
        return remote(chunk(beside, d), chunk(beside, d), x_s.at[1, d], x_r.at[1, d], across_x)

    def kv_copy(i, d):
        src, dst = stream[i]
        block = lax.rem(z - d + groups, groups) * 2 + y
        return remote(
            src if d == 0 else dst.at[block], dst.at[block], kvy_s.at[i, d], kvy_r.at[i, d], across_y
        )

    @pl.when(y == 0)
    def _():
        for i in range(3):
            kv_copy(i, 0).start()

    y_copy(0).start()
    x_copy(0).start()
    weights = [
        remote(src, dst, w_s.at[i], w_r.at[i], across_c)
        for i, (src, dst) in enumerate(((gate, gate_o), (up, up_o), (down, down_o)))
    ]
    for copy in weights:
        copy.start()
    locals_ = [
        pltpu.make_async_copy(src, dst.at[ep], local_sem.at[i])
        for i, (src, dst) in enumerate(stream)
    ] + [pltpu.make_async_copy(slots.at[z], rows.at[own, z], local_sem.at[3])]
    for copy in locals_:
        copy.start()

    for d in range(1, groups):
        @pl.when(z >= d)
        def _(d=d):
            for i, (src, dst) in enumerate(stream):
                remote(src, dst.at[ep], kvz_s.at[i, d], kvz_r.at[i, d], across_y).wait_recv()
                kv_copy(i, d).start()

        y_copy(d - 1).wait_recv()
        x_relay(d - 1).start()
        z_copy(d).wait_recv()
        y_copy(d).start()
        x_copy(d).start()
    y_copy(groups - 1).wait_recv()
    x_relay(groups - 1).start()

    for copy in locals_:
        copy.wait()
    for copy in weights:
        copy.wait()
    for i in range(3):
        @pl.when(y == 1)
        def _(i=i):
            kv_copy(i, 0).wait_recv()

        @pl.when(y == 0)
        def _(i=i):
            kv_copy(i, 0).wait_send()

        for d in range(1, groups):
            @pl.when(z >= d)
            def _(i=i, d=d):
                kv_copy(i, d).wait()

            @pl.when(z + d < groups)
            def _(i=i, d=d):
                src, dst = stream[i]
                remote(src, dst.at[ep], kvz_s.at[i, d], kvz_r.at[i, d], across_y).wait_send()

    for d in range(groups):
        if d:
            z_copy(d).wait_send()
        y_copy(d).wait_send()
        x_copy(d).wait()
        x_relay(d).wait()


def dispatch(slots, keys, vals, cum, gate, up, down, ep_count):
    groups, cap, width = slots.shape
    dma = pltpu.SemaphoreType.DMA
    like = lambda a: jax.ShapeDtypeStruct(a.shape, a.dtype)
    many = lambda a: jax.ShapeDtypeStruct((ep_count,) + a.shape, a.dtype)
    return pl.pallas_call(
        functools.partial(dispatch_kernel, groups),
        name="dispatch",
        out_shape=(
            jax.ShapeDtypeStruct((4, groups, cap, width), slots.dtype),
            many(keys), many(vals), many(cum), like(gate), like(up), like(down),
        ),
        in_specs=[VMEM] * 4 + [ANY] * 3,
        out_specs=(ANY,) * 7,
        scratch_shapes=[
            dma((4,)), dma((3, groups)), dma((3, groups)), dma((3, groups)), dma((3, groups)),
            dma((3,)), dma((3,)), dma((groups,)), dma((groups,)), dma((groups,)), dma((groups,)),
            dma((2, groups)), dma((2, groups)),
        ],
        compiler_params=pltpu.CompilerParams(
            collective_id=0, has_side_effects=True, vmem_limit_bytes=8 * 1024 * 1024
        ),
    )(slots, keys, vals, cum, gate, up, down)


def collect_kernel(
    groups, part, mix, ret, mixed,
    xr, ysum, yr, zsum, mr, msum, mx,
    local_sem, x_s, x_r, y_s, y_r, z_s, z_r, c_s, c_r, m_s, m_r,
):
    ep, tp, z, y, x, c = places()
    greet(groups)
    across_y = (z * 2 + 1 - y, tp)
    across_x = (ep, (1 - x) * 2 + c)
    across_c = (ep, x * 2 + 1 - c)

    def to_of(d):
        return lax.rem(z + d, groups)

    def c_copy(i):
        return remote(mix.at[i, 1 - c], mr.at[i], c_s.at[i], c_r.at[i], across_c)

    def x_copy(i, d):
        column = 1 - y if i == 0 else y
        return remote(
            part.at[1 - x, column, to_of(d)], xr.at[i, d], x_s.at[i, d], x_r.at[i, d], across_x
        )

    def y_copy(d):
        return remote(ysum.at[d], yr.at[d], y_s.at[d], y_r.at[d], across_y)

    def z_copy(d):
        return remote(zsum.at[d], ret.at[z], z_s.at[d], z_r.at[d], (to_of(d) * 2 + y, tp))

    m_copy = remote(msum, mx, m_s, m_r, across_x)
    local = pltpu.make_async_copy(zsum.at[0], ret.at[z], local_sem)
    order = list(range(1, groups)) + [0]
    for i in range(2):
        c_copy(i).start()
    for d in order:
        x_copy(0, d).start()
        x_copy(1, d).start()
    for i in range(2):
        c_copy(i).wait_recv()
    f32 = jnp.float32
    msum[...] = (mix[1 - x, c].astype(f32) + mr[1 - x].astype(f32)).astype(msum.dtype)
    m_copy.start()
    for step, d in enumerate(order):
        x_copy(0, d).wait_recv()
        ysum[d] = (part[x, 1 - y, to_of(d)].astype(f32) + xr[0, d].astype(f32)).astype(ysum.dtype)
        y_copy(d).start()
        for last in ([order[step - 1]] if step else []) + ([d] if step == groups - 1 else []):
            x_copy(1, last).wait_recv()
            y_copy(last).wait_recv()
            zsum[last] = (
                part[x, y, to_of(last)].astype(f32) + xr[1, last].astype(f32) + yr[last].astype(f32)
            ).astype(zsum.dtype)
            if last:
                z_copy(last).start()
            else:
                local.start()
    m_copy.wait_recv()
    mixed[...] = mix[x, c].astype(f32) + mr[x].astype(f32) + mx[...].astype(f32)
    local.wait()
    m_copy.wait_send()
    for i in range(2):
        c_copy(i).wait_send()
    for d in range(groups):
        x_copy(0, d).wait_send()
        x_copy(1, d).wait_send()
        y_copy(d).wait_send()
        if d:
            z_copy(d).wait()


def collect(part, mix):
    groups, cap, width = part.shape[2:]
    own = mix.shape[2]
    dma = pltpu.SemaphoreType.DMA
    bf16 = jnp.bfloat16
    return pl.pallas_call(
        functools.partial(collect_kernel, groups),
        name="collect",
        out_shape=(
            jax.ShapeDtypeStruct((groups, cap, width), bf16),
            jax.ShapeDtypeStruct((own, width), jnp.float32),
        ),
        in_specs=[VMEM] * 2,
        out_specs=(VMEM,) * 2,
        scratch_shapes=[
            pltpu.VMEM((2, groups, cap, width), bf16),
            pltpu.VMEM((groups, cap, width), bf16),
            pltpu.VMEM((groups, cap, width), bf16),
            pltpu.VMEM((groups, cap, width), bf16),
            pltpu.VMEM((2, own, width), bf16),
            pltpu.VMEM((own, width), bf16),
            pltpu.VMEM((own, width), bf16),
            dma, dma((2, groups)), dma((2, groups)), dma((groups,)), dma((groups,)),
            dma((groups,)), dma((groups,)), dma((2,)), dma((2,)), dma, dma,
        ],
        compiler_params=pltpu.CompilerParams(
            collective_id=1, has_side_effects=True, vmem_limit_bytes=40 * 1024 * 1024
        ),
    )(part, mix)


def attend_kernel(ratio, tile, place, q_ref, k_ref, v_ref, cum_ref, qcum_ref, w_ref, out_ref):
    ep = place[0]
    rows, heads = qcum_ref.shape
    f32 = jnp.float32
    nt = (((1,), (1,)), ((), ()))
    for start in range(0, rows, tile):
        done = []
        for h in range(heads):
            head = slice((h // ratio) * DH, (h // ratio + 1) * DH)
            q = q_ref[start : start + tile, h * DH : (h + 1) * DH]
            qcum = qcum_ref[start : start + tile, h : h + 1] * LOG2E
            width = start + tile

            def weigh(s, bias, block, length):
                v = v_ref[block, :length, head]
                return jnp.dot(s.astype(jnp.bfloat16), v, preferred_element_type=f32)

            s = lax.dot_general(q, k_ref[ep, :width, head], nt, preferred_element_type=f32)
            s = s * (LOG2E / math.sqrt(DH)) + (qcum - cum_ref[ep, h : h + 1, :width] * LOG2E)
            r = lax.broadcasted_iota(jnp.int32, s.shape, 0) + start
            k = lax.broadcasted_iota(jnp.int32, s.shape, 1)
            s = jnp.where(k <= r, s, -1e30)
            top = jnp.max(s, axis=1, keepdims=True)
            e = jnp.exp2(s - top)
            total = jnp.sum(e, axis=1, keepdims=True)
            acc = weigh(e, None, ep, width)

            def step(i, state):
                top, total, acc, gap = state
                j = ep - 1 - i
                gap = gap + cum_ref[j, h : h + 1, rows - 1 : rows] * LOG2E
                s = lax.dot_general(q, k_ref[j, :, head], nt, preferred_element_type=f32)
                s = s * (LOG2E / math.sqrt(DH)) + (
                    qcum + (gap - cum_ref[j, h : h + 1, :] * LOG2E)
                )
                new = jnp.maximum(top, jnp.max(s, axis=1, keepdims=True))
                e = jnp.exp2(s - new)
                scale = jnp.exp2(top - new)
                total = total * scale + jnp.sum(e, axis=1, keepdims=True)
                return new, total, acc * scale + weigh(e, None, j, rows), gap

            top, total, acc, _ = lax.fori_loop(
                0, ep, step, (top, total, acc, jnp.zeros((1, 1), f32))
            )
            done.append((acc / total).astype(jnp.bfloat16))
        attended = jnp.concatenate(done, axis=1)
        out_ref[start : start + tile, :] = jnp.dot(
            attended, w_ref[...], preferred_element_type=f32
        ).astype(out_ref.dtype)


def attend(place, queries, keys_all, vals_all, cum_all, qcum, out_weight, ratio):
    rows = queries.shape[0]
    return pl.pallas_call(
        functools.partial(attend_kernel, ratio, math.gcd(rows, 256)),
        name="attend",
        out_shape=jax.ShapeDtypeStruct((rows, out_weight.shape[1]), jnp.bfloat16),
        in_specs=[pl.BlockSpec(memory_space=pltpu.SMEM)] + [VMEM] * 6,
        out_specs=VMEM,
        compiler_params=pltpu.CompilerParams(vmem_limit_bytes=40 * 1024 * 1024),
    )(place, queries, keys_all, vals_all, cum_all, qcum, out_weight)


def expert_kernel(place, rows, gate, gate_o, up, up_o, down, down_o, router, out):
    expert = place[0]
    group = expert // 2
    f32 = jnp.float32
    block = rows[...]
    dot = lambda a, b: jnp.dot(a, b[...], preferred_element_type=f32)
    logits = dot(block, router)
    lane = lax.broadcasted_iota(jnp.int32, logits.shape, 1)
    pick = lambda index: jnp.sum(jnp.where(lane == index, logits, 0.0), axis=1, keepdims=True)
    in_group = lane < GROUPS
    top = jnp.max(jnp.where(in_group, logits, -jnp.inf), axis=1, keepdims=True)
    total = jnp.sum(jnp.where(in_group, jnp.exp(logits - top), 0.0), axis=1, keepdims=True)
    other = expert + 1 - 2 * (expert % 2)
    share = jnp.exp(pick(group) - top) / total
    share = share * jax.nn.sigmoid(pick(GROUPS + expert) - pick(GROUPS + other))
    result = None
    for g, u, w in ((gate, up, down), (gate_o, up_o, down_o)):
        hidden = (jax.nn.silu(dot(block, g)) * dot(block, u)).astype(jnp.bfloat16)
        term = dot(hidden, w)
        result = term if result is None else result + term
    out[...] = (share * result).astype(out.dtype)


def run_experts(place, rows, gate, gate_o, up, up_o, down, down_o, router):
    count, width = rows.shape
    tile = math.gcd(count, 256)
    full = lambda a: pl.BlockSpec(a.shape, lambda i: (0, 0), pipeline_mode=pl.Buffered(1))
    return pl.pallas_call(
        expert_kernel,
        name="experts",
        grid=(count // tile,),
        out_shape=jax.ShapeDtypeStruct((count, width), jnp.bfloat16),
        in_specs=[
            pl.BlockSpec(memory_space=pltpu.SMEM),
            pl.BlockSpec((tile, width), lambda i: (i, 0)),
        ]
        + [full(a) for a in (gate, gate_o, up, up_o, down, down_o, router)],
        out_specs=pl.BlockSpec((tile, width), lambda i: (i, 0)),
        compiler_params=pltpu.CompilerParams(vmem_limit_bytes=48 * 1024 * 1024),
    )(place, rows, gate, gate_o, up, up_o, down, down_o, router)


def paired_body(
    queries, key_rows, value_rows, forget_logit, out_weight, out_gain, moe_input, moe_gain,
    router_group, router_expert, route_group, route_pick, expert_gate, expert_up, expert_down,
):
    tp_count = lax.axis_size("tp")
    ep_count = lax.axis_size("ep")
    tp_index = lax.axis_index("tp")
    place = lax.axis_index("ep").reshape(1).astype(jnp.int32)
    own_rows = moe_input.shape[0] // tp_count
    width = moe_input.shape[1]
    experts = expert_gate.shape[0] * ep_count
    capacity = tp_count * own_rows // experts
    ratio = forget_logit.shape[0] // (key_rows.shape[1] // DH)
    first = tp_index * own_rows
    local_cum = jnp.cumsum(jax.nn.log_sigmoid(forget_logit), axis=1)
    group = lax.dynamic_slice_in_dim(route_group, first, own_rows, 0)
    normed = rms_scale(
        lax.dynamic_slice_in_dim(moe_input, first, own_rows, 0), moe_gain
    ).astype(jnp.bfloat16)
    index = jnp.arange(own_rows, dtype=jnp.int32)
    earlier = (group[:, None] == group[None, :]) & (index[:, None] < index[None, :])
    rank = jnp.sum(earlier.astype(jnp.int32), axis=0)
    slot = jnp.where(rank < capacity, group * capacity + rank, -1)
    hot = (jnp.arange(GROUPS * capacity, dtype=jnp.int32)[:, None] == slot[None, :]).astype(
        jnp.bfloat16
    )
    slots = jnp.dot(hot, normed, preferred_element_type=jnp.float32).astype(jnp.bfloat16)
    rows, keys_all, vals_all, cum_all, gate_o, up_o, down_o = dispatch(
        slots.reshape(GROUPS, capacity, width), key_rows, value_rows, local_cum,
        expert_gate[0], expert_up[0], expert_down[0], ep_count,
    )
    mix = attend(place, queries, keys_all, vals_all, cum_all, local_cum.T, out_weight, ratio)
    router = jnp.concatenate([router_group, router_expert], axis=1)
    router = jnp.pad(router, ((0, 0), (0, -router.shape[1] % 128)))
    part = run_experts(
        place, rows.reshape(-1, width), expert_gate[0], gate_o, expert_up[0], up_o,
        expert_down[0], down_o, router,
    )
    returned, mixed = collect(
        part.reshape(2, 2, GROUPS, capacity, width), mix.reshape(2, 2, own_rows, width)
    )
    mixer_out = rms_scale(mixed, out_gain).astype(jnp.bfloat16)
    moe_out = lax.dot_general(
        hot, returned.reshape(-1, width), (((0,), (0,)), ((), ())),
        preferred_element_type=jnp.float32,
    )
    return (mixer_out, moe_out.astype(jnp.bfloat16))


def body(*args):
    experts = args[12].shape[0] * lax.axis_size("ep")
    if experts == 2 * GROUPS and args[12].shape[0] == 1 and lax.axis_size("tp") == 4:
        return paired_body(*args)
    return general_body(*args)


def solution(mesh):
    in_specs = (
        P("ep", "tp"),
        P("ep", "tp"),
        P("ep", "tp"),
        P("tp", "ep"),
        P("tp", None),
        P(),
        P("ep", None),
        P(),
        P(),
        P(),
        P("ep"),
        P("ep", None),
        P("ep", None, "tp"),
        P("ep", None, "tp"),
        P("ep", "tp", None),
    )
    out_specs = (P(("ep", "tp"), None), P(("ep", "tp"), None))
    return jax.shard_map(body, mesh=mesh, in_specs=in_specs, out_specs=out_specs, check_vma=False)
```

```python
import functools
import math

import jax
import jax.numpy as jnp
from jax import lax
from jax.experimental import pallas as pl
from jax.experimental.pallas import tpu as pltpu
from jax.sharding import PartitionSpec as P

DH = 128
GROUPS = 4


def rms_scale(row_block, scale_gain):
    values = row_block.astype(jnp.float32)
    return (
        values * lax.rsqrt(jnp.mean(values * values, axis=-1, keepdims=True) + 1e-06) * scale_gain
    )


def slot_ranks(chosen, block_rows, experts):
    expert_ids = jnp.arange(experts, dtype=jnp.int32)
    matches = chosen[:, :, None] == expert_ids
    usage = jnp.any(matches, axis=1).astype(jnp.int32)
    grouped = usage.reshape(-1, block_rows, experts)
    before = (jnp.cumsum(grouped, axis=1) - grouped).reshape(-1, experts)
    return jnp.sum(jnp.where(matches, before[:, None, :], 0), axis=2)


def expert_hidden(arrived, gate_part, up_part):
    flat = arrived.reshape(-1, arrived.shape[-1])
    gated = jnp.dot(flat, gate_part, preferred_element_type=jnp.float32)
    lifted = jnp.dot(flat, up_part, preferred_element_type=jnp.float32)
    hidden = (jax.nn.silu(gated) * lifted).astype(jnp.bfloat16)
    return hidden.reshape(arrived.shape[:-1] + (gate_part.shape[1],))


def general_body(
    queries,
    key_rows,
    value_rows,
    forget_logit,
    out_weight,
    out_gain,
    moe_input,
    moe_gain,
    router_group,
    router_expert,
    route_group,
    route_pick,
    expert_gate,
    expert_up,
    expert_down,
):
    tp_count = lax.axis_size("tp")
    ep_count = lax.axis_size("ep")
    tp_index = lax.axis_index("tp")
    ep_index = lax.axis_index("ep")
    rows_group = queries.shape[0]
    query_heads = forget_logit.shape[0]
    key_heads = key_rows.shape[1] // DH
    ratio = query_heads // key_heads
    own_start = ep_index * rows_group
    own_pos = own_start + jnp.arange(rows_group, dtype=jnp.int32)
    local_cum = jnp.cumsum(jax.nn.log_sigmoid(forget_logit), axis=1)
    every_cum = lax.all_gather(local_cum, "ep", axis=1, tiled=True).reshape(
        query_heads, ep_count, rows_group
    )
    shard_totals = every_cum[:, :, -1]
    offsets = jnp.cumsum(shard_totals, axis=1) - shard_totals
    cum_gate = (every_cum + offsets[:, :, None]).reshape(query_heads, ep_count * rows_group)
    own_cum = lax.dynamic_slice_in_dim(cum_gate, own_start, rows_group, 1).reshape(
        key_heads, ratio, rows_group, 1
    )
    query_stack = (
        queries.reshape(rows_group, key_heads, ratio, DH)
        .transpose(1, 2, 0, 3)
        .reshape(key_heads, ratio * rows_group, DH)
    )

    def attend_block(current, keys_block, values_block, start):
        piece_rows = keys_block.shape[0]

        def compute(state):
            row_top, row_total, weighted = state
            key_stack = keys_block.reshape(piece_rows, key_heads, DH).transpose(1, 0, 2)
            value_stack = values_block.reshape(piece_rows, key_heads, DH).transpose(1, 0, 2)
            scores = jnp.einsum(
                "gqd,gkd->gqk", query_stack, key_stack, preferred_element_type=jnp.float32
            ) / math.sqrt(DH)
            key_cum = lax.dynamic_slice_in_dim(cum_gate, start, piece_rows, 1).reshape(
                key_heads, ratio, 1, piece_rows
            )
            logits = scores.reshape(key_heads, ratio, rows_group, piece_rows) + own_cum - key_cum
            visible = (start + jnp.arange(piece_rows, dtype=jnp.int32))[None, :] <= own_pos[:, None]
            logits = jnp.where(visible, logits, -1e30)
            new_top = jnp.maximum(row_top, jnp.max(logits, axis=3))
            expo = jnp.where(visible, jnp.exp(logits - new_top[..., None]), 0.0)
            rescale = jnp.exp(row_top - new_top)
            row_total = row_total * rescale + jnp.sum(expo, axis=3)
            product = jnp.einsum(
                "gqk,gkd->gqd",
                expo.reshape(key_heads, ratio * rows_group, piece_rows).astype(jnp.bfloat16),
                value_stack,
                preferred_element_type=jnp.float32,
            )
            weighted = weighted * rescale.reshape(key_heads, ratio * rows_group, 1) + product
            return (new_top, row_total, weighted)

        return lax.cond(start < own_start + rows_group, compute, lambda state: state, current)

    initial = (
        jnp.full((key_heads, ratio, rows_group), -1e30, jnp.float32),
        jnp.zeros((key_heads, ratio, rows_group), jnp.float32),
        jnp.zeros((key_heads, ratio * rows_group, DH), jnp.float32),
    )
    current = initial
    keys_piece = lax.all_gather(key_rows, "ep", axis=0, tiled=True)
    values_piece = lax.all_gather(value_rows, "ep", axis=0, tiled=True)
    piece_rows = keys_piece.shape[0]
    blocks = piece_rows // rows_group

    def advance(state, inputs):
        keys_block, values_block, block_index = inputs
        return (attend_block(state, keys_block, values_block, block_index * rows_group), None)

    current, _ = lax.scan(
        advance,
        current,
        (
            keys_piece.reshape(blocks, rows_group, -1),
            values_piece.reshape(blocks, rows_group, -1),
            jnp.arange(blocks, dtype=jnp.int32),
        ),
    )
    row_top, row_total, weighted = current
    attended = (weighted / row_total.reshape(key_heads, ratio * rows_group, 1)).astype(jnp.bfloat16)
    attended = (
        attended.reshape(key_heads, ratio, rows_group, DH)
        .transpose(2, 0, 1, 3)
        .reshape(rows_group, query_heads * DH)
    )
    group_rows = moe_input.shape[0]
    own_rows = group_rows // tp_count
    width_model = moe_input.shape[1]
    experts = expert_gate.shape[0] * ep_count
    per_group = experts // GROUPS
    capacity = tp_count * own_rows // experts
    own_first = tp_index * own_rows
    chosen_all = route_group[:, None] * per_group + route_pick
    rank_all = slot_ranks(chosen_all, own_rows, experts)
    chosen = lax.dynamic_slice_in_dim(chosen_all, own_first, own_rows, 0)
    ranks = lax.dynamic_slice_in_dim(rank_all, own_first, own_rows, 0)
    is_kept = ranks < capacity
    own_group = lax.dynamic_slice_in_dim(route_group, own_first, own_rows, 0)
    normed = rms_scale(
        lax.dynamic_slice_in_dim(moe_input, own_first, own_rows, 0), moe_gain
    ).astype(jnp.bfloat16)
    target = jnp.where(is_kept, chosen * capacity + ranks, experts * capacity)
    sources = jnp.broadcast_to(jnp.arange(own_rows, dtype=jnp.int32)[:, None], target.shape)
    slot_table = (
        jnp.full((experts * capacity,), own_rows, jnp.int32)
        .at[target.reshape(-1)]
        .set(sources.reshape(-1), mode="drop")
    )
    padded = jnp.concatenate([normed, jnp.zeros((1, width_model), jnp.bfloat16)], axis=0)
    outgoing = padded[slot_table].reshape(experts, capacity, width_model)
    arrived = lax.all_to_all(outgoing, "ep", split_axis=0, concat_axis=0, tiled=True)
    hidden_arrived = lax.all_gather(arrived[None], "tp", axis=0, tiled=True)
    hidden = expert_hidden(hidden_arrived, expert_gate[0], expert_up[0])
    hidden_rows = hidden.reshape(-1, hidden.shape[-1])
    mixer_term = jnp.dot(attended, out_weight, preferred_element_type=jnp.float32)
    expert_term = jnp.dot(hidden_rows, expert_down[0], preferred_element_type=jnp.float32)
    mixer_summed, expert_summed = (
        lax.psum_scatter(
            mixer_term.astype(jnp.bfloat16), "tp", scatter_dimension=0, tiled=True
        ).astype(jnp.float32),
        lax.psum_scatter(
            expert_term.astype(jnp.bfloat16), "tp", scatter_dimension=0, tiled=True
        ).astype(jnp.float32),
    )
    mixer_out = rms_scale(mixer_summed, out_gain).astype(jnp.bfloat16)
    group_logits = jnp.dot(normed, router_group, preferred_element_type=jnp.float32)
    expert_logits = jnp.dot(normed, router_expert, preferred_element_type=jnp.float32)
    group_top = jnp.max(group_logits, axis=1, keepdims=True)
    group_exp = jnp.exp(group_logits - group_top)
    group_hit = jnp.arange(GROUPS, dtype=jnp.int32)[None, :] == own_group[:, None]
    group_share = jnp.sum(jnp.where(group_hit, group_exp, 0.0), axis=1) / jnp.sum(group_exp, axis=1)
    expert_hit = jnp.arange(experts, dtype=jnp.int32)[None, None, :] == chosen[:, :, None]
    picked_logits = jnp.sum(jnp.where(expert_hit, expert_logits[:, None, :], 0.0), axis=2)
    shares = group_share[:, None] * jax.nn.sigmoid(picked_logits - picked_logits[:, ::-1])
    results = expert_summed.astype(jnp.bfloat16).reshape(ep_count, capacity, width_model)
    returned = lax.all_to_all(results, "ep", split_axis=0, concat_axis=0, tiled=True).reshape(
        experts * capacity, width_model
    )
    slot_index = jnp.where(is_kept, chosen * capacity + ranks, 0)
    picked = returned[slot_index]
    moe_out = jnp.sum(
        jnp.where(is_kept, shares, 0.0)[:, :, None] * picked.astype(jnp.float32), axis=1
    )
    return (mixer_out, moe_out.astype(jnp.bfloat16))


LOG2E = math.log2(math.e)
MESH = pl.DeviceIdType.MESH
VMEM = pl.BlockSpec(memory_space=pltpu.VMEM)
ANY = pl.BlockSpec(memory_space=pl.ANY)


def places():
    ep, tp = lax.axis_index("ep"), lax.axis_index("tp")
    return ep, tp, ep // 2, ep % 2, tp // 2, tp % 2


def greet(groups):
    ep, tp, z, y, x, c = places()
    barrier = pltpu.get_barrier_semaphore()
    peers = [(z * 2 + 1 - y, tp), (ep, (1 - x) * 2 + c), (ep, x * 2 + 1 - c)]
    peers += [(lax.rem(z + d, groups) * 2 + y, tp) for d in range(1, groups)]
    for peer in peers:
        pl.semaphore_signal(barrier, inc=1, device_id=peer, device_id_type=MESH)
    pl.semaphore_wait(barrier, len(peers))


def remote(src, dst, send, recv, peer):
    return pltpu.make_async_remote_copy(
        src_ref=src, dst_ref=dst, send_sem=send, recv_sem=recv, device_id=peer, device_id_type=MESH
    )


def attend_tile(ratio, start, tile, ep, q_ref, k_ref, v_ref, cum_ref, qcum_ref):
    rows, heads = qcum_ref.shape
    f32 = jnp.float32
    nt = (((1,), (1,)), ((), ()))
    done = []
    for h in range(heads):
        head = slice((h // ratio) * DH, (h // ratio + 1) * DH)
        q = q_ref[start : start + tile, h * DH : (h + 1) * DH]
        qcum = qcum_ref[start : start + tile, h : h + 1] * LOG2E
        width = start + tile
        s = lax.dot_general(q, k_ref[ep, :width, head], nt, preferred_element_type=f32)
        s = s * (LOG2E / math.sqrt(DH)) + (qcum - cum_ref[ep, h : h + 1, :width] * LOG2E)
        r = lax.broadcasted_iota(jnp.int32, s.shape, 0) + start
        k = lax.broadcasted_iota(jnp.int32, s.shape, 1)
        s = jnp.where(k <= r, s, -1e30)
        top = jnp.max(s, axis=1, keepdims=True)
        e = jnp.exp2(s - top)
        total = jnp.sum(e, axis=1, keepdims=True)
        acc = jnp.dot(e.astype(jnp.bfloat16), v_ref[ep, :width, head], preferred_element_type=f32)

        def step(i, state):
            top, total, acc, gap = state
            j = ep - 1 - i
            gap = gap + cum_ref[j, h : h + 1, rows - 1 : rows] * LOG2E
            s = lax.dot_general(q, k_ref[j, :, head], nt, preferred_element_type=f32)
            s = s * (LOG2E / math.sqrt(DH)) + (qcum + (gap - cum_ref[j, h : h + 1, :] * LOG2E))
            new = jnp.maximum(top, jnp.max(s, axis=1, keepdims=True))
            e = jnp.exp2(s - new)
            scale = jnp.exp2(top - new)
            total = total * scale + jnp.sum(e, axis=1, keepdims=True)
            acc = acc * scale + jnp.dot(
                e.astype(jnp.bfloat16), v_ref[j, :, head], preferred_element_type=f32
            )
            return new, total, acc, gap

        top, total, acc, _ = lax.fori_loop(0, ep, step, (top, total, acc, jnp.zeros((1, 1), f32)))
        done.append((acc / total).astype(jnp.bfloat16))
    return jnp.concatenate(done, axis=1)


def expert_rows(expert, block, router, weights):
    f32 = jnp.float32
    group = expert // 2
    dot = lambda a, b: jnp.dot(a, b[...], preferred_element_type=f32)
    logits = lax.dot_general(
        block, router[...], (((1,), (1,)), ((), ())), preferred_element_type=f32
    )
    lane = lax.broadcasted_iota(jnp.int32, logits.shape, 1)
    pick = lambda index: jnp.sum(jnp.where(lane == index, logits, 0.0), axis=1, keepdims=True)
    in_group = lane < GROUPS
    top = jnp.max(jnp.where(in_group, logits, -jnp.inf), axis=1, keepdims=True)
    total = jnp.sum(jnp.where(in_group, jnp.exp(logits - top), 0.0), axis=1, keepdims=True)
    other = expert + 1 - 2 * (expert % 2)
    share = jnp.exp(pick(group) - top) / total
    share = share * jax.nn.sigmoid(pick(GROUPS + expert) - pick(GROUPS + other))
    result = None
    for g, u, w in weights:
        hidden = (jax.nn.silu(dot(block, g)) * dot(block, u)).astype(jnp.bfloat16)
        term = dot(hidden, w)
        result = term if result is None else result + term
    return (share * result).astype(jnp.bfloat16)


def main_kernel(
    groups, ratio,
    slots, keys, vals, cum, gate, up, down, queries, out_weight, qcum, router,
    ret, mixed,
    rows, keys_all, vals_all, cum_all, gate_i, up_i, down_i, gate_o, up_o, down_o, q_v, w_v,
    part, xr, ysum, yr, zsum, mix, mr, msum, mx,
    local_sem, ret_sem, kvz_s, kvz_r, kvy_s, kvy_r, w_s, w_r, z_s, z_r, y_s, y_r, x_s, x_r, e_s, e_r,
    bx_s, bx_r, by_s, by_r, bz_s, bz_r, c_s, c_r, m_s, m_r,
):
    ep, tp, z, y, x, c = places()
    f32 = jnp.float32
    greet(groups)
    across_y = (z * 2 + 1 - y, tp)
    across_x = (ep, (1 - x) * 2 + c)
    across_c = (ep, x * 2 + 1 - c)
    own = x * 2 + y
    by_y = x * 2 + 1 - y
    by_x = (1 - x) * 2 + y
    stream = ((keys, keys_all), (vals, vals_all), (cum, cum_all))
    far = lambda d: d % 2 == 1

    def origin(d):
        return lax.rem(z - d + groups, groups)

    def z_copy(d):
        to = lax.rem(z + d, groups)
        return remote(slots.at[to], rows.at[z, own], z_s.at[d], z_r.at[d], (to * 2 + y, tp))

    def piece(q, d):
        return rows.at[origin(d), q]

    def y_copy(d):
        src = slots.at[z] if d == 0 else piece(own, d)
        return remote(src, piece(own, d), y_s.at[d], y_r.at[d], across_y)

    def x_copy(d):
        src = slots.at[z] if d == 0 else piece(own, d)
        return remote(src, piece(own, d), x_s.at[d], x_r.at[d], across_x)

    def relay(d):
        q, to = (by_x, across_y) if far(d) else (by_y, across_x)
        return remote(piece(q, d), piece(q, d), e_s.at[d], e_r.at[d], to)

    def kvz_copy(i, d):
        src, dst = stream[i]
        to = (lax.rem(z + d, groups) * 2 + y, tp)
        return remote(src, dst.at[ep], kvz_s.at[i, d], kvz_r.at[i, d], to)

    def kvy_copy(i, d):
        src, dst = stream[i]
        block = origin(d) * 2 + y
        return remote(
            src if d == 0 else dst.at[block], dst.at[block], kvy_s.at[i, d], kvy_r.at[i, d], across_y
        )

    def c_copy(i):
        return remote(mix.at[i, 1 - c], mr.at[i], c_s.at[i], c_r.at[i], across_c)

    def back_x(i, d):
        q = (1 - x) * 2 + (1 - y if i == 0 else y)
        return remote(piece_out(q, d), xr.at[i, d], bx_s.at[i, d], bx_r.at[i, d], across_x)

    def piece_out(q, d):
        return part.at[origin(d), q]

    def back_y(d):
        return remote(ysum.at[d], yr.at[d], by_s.at[d], by_r.at[d], across_y)

    def back_z(d):
        to = (origin(d) * 2 + y, tp)
        return remote(zsum.at[d], ret.at[z], bz_s.at[d], bz_r.at[d], to)

    y_copy(0).start()
    x_copy(0).start()
    z_copy(1).start()
    for d in range(1, groups):
        @pl.when(z + d < groups)
        def _(d=d):
            for i in range(3):
                kvz_copy(i, d).start()

    for d in range(2, groups):
        z_copy(d).start()

    @pl.when(y == 0)
    def _():
        for i in range(3):
            kvy_copy(i, 0).start()

    loads = (
        (slots.at[z], piece(own, 0)), (gate, gate_i), (up, up_i), (down, down_i),
        (keys, keys_all.at[ep]), (vals, vals_all.at[ep]), (cum, cum_all.at[ep]),
        (queries, q_v), (out_weight, w_v),
    )
    loads = [pltpu.make_async_copy(src, dst, local_sem.at[i]) for i, (src, dst) in enumerate(loads)]
    swaps = [
        remote(src, dst, w_s.at[i], w_r.at[i], across_c)
        for i, (src, dst) in enumerate(((gate, gate_o), (up, up_o), (down, down_o)))
    ]
    for copy in loads + swaps:
        copy.start()

    def pass_on(d):
        z_copy(d).wait_recv()
        y_copy(d).start()
        x_copy(d).start()

        @pl.when(z >= d)
        def _():
            for i in range(3):
                kvz_copy(i, d).wait_recv()
                kvy_copy(i, d).start()

    def turn(d):
        (x_copy(d) if far(d) else y_copy(d)).wait_recv()
        relay(d).start()

    def experts(d):
        (y_copy(d) if far(d) else x_copy(d)).wait_recv()
        relay(d).wait_recv()
        at = origin(d)
        block = rows[at].reshape(-1, rows.shape[-1])
        out = expert_rows(ep, block, router, ((gate_i, up_i, down_i), (gate_o, up_o, down_o)))
        part[at] = out.reshape(rows.shape[1:])
        back_x(0, d).start()
        back_x(1, d).start()

    def fold_x(d):
        back_x(0, d).wait_recv()
        ysum[d] = (part[origin(d), by_y].astype(f32) + xr[0, d].astype(f32)).astype(ysum.dtype)
        back_y(d).start()

    home = pltpu.make_async_copy(zsum.at[0], ret.at[z], ret_sem)

    def fold_y(d):
        back_x(1, d).wait_recv()
        back_y(d).wait_recv()
        zsum[d] = (
            part[origin(d), own].astype(f32) + xr[1, d].astype(f32) + yr[d].astype(f32)
        ).astype(zsum.dtype)
        if d:
            back_z(d).start()
        else:
            home.start()

    pass_on(1)
    turn(0)
    for copy in loads[:4] + swaps:
        copy.wait()
    experts(0)
    pass_on(2)
    turn(1)
    experts(1)
    pass_on(3)
    turn(2)
    fold_x(0)
    turn(3)

    for copy in loads[4:]:
        copy.wait()
    for i in range(3):
        @pl.when(y == 1)
        def _(i=i):
            kvy_copy(i, 0).wait_recv()

        @pl.when(y == 0)
        def _(i=i):
            kvy_copy(i, 0).wait_send()

        for d in range(1, groups):
            @pl.when(z >= d)
            def _(i=i, d=d):
                kvy_copy(i, d).wait()

    experts(2)
    length = qcum.shape[0]
    tile = mix.shape[2]
    for start in range(0, length, 2 * tile):
        attended = attend_tile(
            ratio, start, 2 * tile, ep, q_v, keys_all, vals_all, cum_all, qcum
        )
        out = jnp.dot(attended, w_v[...], preferred_element_type=f32).astype(mix.dtype)
        mix[start // (2 * tile)] = out.reshape(mix.shape[1:])
        c_copy(start // (2 * tile)).start()
        if start == 0:
            fold_x(1)
            fold_y(0)
    m_copy = remote(msum, mx, m_s, m_r, across_x)
    experts(3)
    for i in range(2):
        c_copy(i).wait_recv()
    msum[...] = (mix[1 - x, c].astype(f32) + mr[1 - x].astype(f32)).astype(msum.dtype)
    m_copy.start()
    fold_y(1)
    fold_x(2)
    fold_x(3)
    fold_y(2)
    fold_y(3)
    m_copy.wait_recv()
    mixed[...] = mix[x, c].astype(f32) + mr[x].astype(f32) + mx[...].astype(f32)

    home.wait()
    m_copy.wait_send()
    for i in range(2):
        c_copy(i).wait_send()
    for d in range(groups):
        y_copy(d).wait_send()
        x_copy(d).wait_send()
        relay(d).wait_send()
        back_x(0, d).wait_send()
        back_x(1, d).wait_send()
        back_y(d).wait_send()
        if d:
            z_copy(d).wait_send()
            back_z(d).wait()

            @pl.when(z + d < groups)
            def _(d=d):
                for i in range(3):
                    kvz_copy(i, d).wait_send()


def run_main(slots, keys, vals, cum, gate, up, down, queries, out_weight, qcum, router, ep_count, ratio):
    groups, cap, width = slots.shape
    own = queries.shape[0] // 4
    dma = pltpu.SemaphoreType.DMA
    bf16 = jnp.bfloat16
    same = lambda a: pltpu.VMEM(a.shape, a.dtype)
    many = lambda a: pltpu.VMEM((ep_count,) + a.shape, a.dtype)
    pieces = pltpu.VMEM((groups, cap, width), bf16)
    tile = pltpu.VMEM((own, width), bf16)
    line = dma((groups,))
    return pl.pallas_call(
        functools.partial(main_kernel, groups, ratio),
        name="main",
        out_shape=(
            jax.ShapeDtypeStruct((groups, cap, width), bf16),
            jax.ShapeDtypeStruct((own, width), jnp.float32),
        ),
        in_specs=[ANY] * 9 + [VMEM] * 2,
        out_specs=(VMEM,) * 2,
        scratch_shapes=[
            pltpu.VMEM((groups, 4, cap, width), bf16),
            many(keys), many(vals), many(cum),
            same(gate), same(up), same(down), same(gate), same(up), same(down),
            same(queries), same(out_weight),
            pltpu.VMEM((groups, 4, cap, width), bf16),
            pltpu.VMEM((2, groups, cap, width), bf16),
            pieces, pieces, pieces,
            pltpu.VMEM((2, 2, own, width), bf16),
            pltpu.VMEM((2, own, width), bf16),
            tile, tile,
            dma((9,)), dma, dma((3, groups)), dma((3, groups)), dma((3, groups)), dma((3, groups)),
            dma((3,)), dma((3,)), line, line, line, line, line, line, line, line,
            dma((2, groups)), dma((2, groups)), line, line, line, line,
            dma((2,)), dma((2,)), dma, dma,
        ],
        compiler_params=pltpu.CompilerParams(
            collective_id=0, has_side_effects=True, vmem_limit_bytes=60 * 1024 * 1024
        ),
    )(slots, keys, vals, cum, gate, up, down, queries, out_weight, qcum, router)


def paired_body(
    queries, key_rows, value_rows, forget_logit, out_weight, out_gain, moe_input, moe_gain,
    router_group, router_expert, route_group, route_pick, expert_gate, expert_up, expert_down,
):
    tp_count = lax.axis_size("tp")
    ep_count = lax.axis_size("ep")
    tp_index = lax.axis_index("tp")
    own_rows = moe_input.shape[0] // tp_count
    width = moe_input.shape[1]
    experts = expert_gate.shape[0] * ep_count
    capacity = tp_count * own_rows // experts
    ratio = forget_logit.shape[0] // (key_rows.shape[1] // DH)
    first = tp_index * own_rows
    local_cum = jnp.cumsum(jax.nn.log_sigmoid(forget_logit), axis=1)
    group = lax.dynamic_slice_in_dim(route_group, first, own_rows, 0)
    normed = rms_scale(
        lax.dynamic_slice_in_dim(moe_input, first, own_rows, 0), moe_gain
    ).astype(jnp.bfloat16)
    index = jnp.arange(own_rows, dtype=jnp.int32)
    earlier = (group[:, None] == group[None, :]) & (index[:, None] < index[None, :])
    rank = jnp.sum(earlier.astype(jnp.int32), axis=0)
    slot = jnp.where(rank < capacity, group * capacity + rank, -1)
    hot = (jnp.arange(GROUPS * capacity, dtype=jnp.int32)[:, None] == slot[None, :]).astype(
        jnp.bfloat16
    )
    slots = jnp.dot(hot, normed, preferred_element_type=jnp.float32).astype(jnp.bfloat16)
    router = jnp.concatenate([router_group.T, router_expert.T], axis=0)
    router = jnp.pad(router, ((0, -router.shape[0] % 16), (0, 0)))
    returned, mixed = run_main(
        slots.reshape(GROUPS, capacity, width), key_rows, value_rows, local_cum,
        expert_gate[0], expert_up[0], expert_down[0], queries, out_weight, local_cum.T, router,
        ep_count, ratio,
    )
    mixer_out = rms_scale(mixed, out_gain).astype(jnp.bfloat16)
    moe_out = lax.dot_general(
        hot, returned.reshape(-1, width), (((0,), (0,)), ((), ())),
        preferred_element_type=jnp.float32,
    )
    return (mixer_out, moe_out.astype(jnp.bfloat16))


def body(*args):
    experts = args[12].shape[0] * lax.axis_size("ep")
    if experts == 2 * GROUPS and args[12].shape[0] == 1 and lax.axis_size("tp") == 4:
        return paired_body(*args)
    return general_body(*args)


def solution(mesh):
    in_specs = (
        P("ep", "tp"),
        P("ep", "tp"),
        P("ep", "tp"),
        P("tp", "ep"),
        P("tp", None),
        P(),
        P("ep", None),
        P(),
        P(),
        P(),
        P("ep"),
        P("ep", None),
        P("ep", None, "tp"),
        P("ep", None, "tp"),
        P("ep", "tp", None),
    )
    out_specs = (P(("ep", "tp"), None), P(("ep", "tp"), None))
    return jax.shard_map(body, mesh=mesh, in_specs=in_specs, out_specs=out_specs, check_vma=False)
```
